32 devices in a mesh: sp: 8 (over z, y), dp: 4 (over x, core).
Axes of the slice: x: 2, y: 2, z: 4, core: 2. Of those that a mesh axis runs over, the one named last changes fastest.
Arguments:
- queries: bfloat16 [4, 1024, 1024], P('dp', 'sp'), may hold values from -6 to 6
- keys: bfloat16 [4, 1024, 1024], P('dp', 'sp'), may hold values from -6 to 6
- values: bfloat16 [4, 1024, 2048], P('dp', 'sp'), may hold values from -6 to 6
- decay_in: bfloat16 [4, 1024, 16], P('dp', 'sp'), may hold values from -1 to 2048
- mix_in: bfloat16 [4, 1024, 16], P('dp', 'sp'), may hold values from -6 to 6
- rates: float32 [16], replicated, may hold values from 0 to 1, as said below
- head_gain: float32 [128], replicated, may hold values from 0.1 to 1.9
- out_weight: bfloat16 [2048, 2048], replicated, may hold values from -0.125 to 0.125
- residual: bfloat16 [4, 1024, 2048], P('dp', 'sp'), may hold values from -6 to 6
- mix_gain: float32 [2048], replicated, may hold values from 0.1 to 1.9
- ffn_gain: float32 [2048], replicated, may hold values from 0.1 to 1.9
- route: int32 [4, 1024, 2], P('dp', 'sp'), may hold values from 0 to 31, all different within a row; in each aligned block of 128 rows (0 to 127, 128 to 255, ..., all dimensions but the last counted through in order) at most 16 rows name the same one
- route_weight: float32 [4, 1024, 2], P('dp', 'sp'), may hold values from 0.1 to 1
- w_gate: bfloat16 [32, 2048, 512], P(('sp', 'dp')), may hold values from -0.125 to 0.125
- w_up: bfloat16 [32, 2048, 512], P(('sp', 'dp')), may hold values from -0.125 to 0.125
- w_down: bfloat16 [32, 512, 2048], P(('sp', 'dp')), may hold values from -0.25 to 0.25
- out_gain: float32 [2048], replicated, may hold values from 0.1 to 1.9
Outputs:
- mixed: bfloat16 [4, 1024, 2048], P('dp', 'sp')
The draws below stay inside these ranges and needn't reach their ends.
Inputs may be any that keep to these rules, and one draw needn't show every extreme that they name: `route`: in the rows of one device no expert is named by more than 16 rows, and one is named by exactly 16; a row names 2 different experts. `rates`: Positive.
All inputs are finite; a program needn't handle non-finite values.
Results may differ from the reference program's by a relative error of at most 0.015.
Values may be sent and summed in bfloat16 or wider, within the bound.
A program may use at most 128 MiB of HBM per device.

```python
import math
import jax
import jax.numpy as jnp
import numpy as np
from jax import lax

D = 2048
HEADS = 16
DK = 64
DV = 128
FF = 512
TOPK = 2
BLOCK = 128
TOK_DEV = 128
SEQ = 1024
SEQS = 4
EXPERTS = 32
CAP = 16


def rate_table(key):
    base = jax.random.fold_in(key, 101)
    pick_key, slow_key, quick_key = jax.random.split(base, 3)
    share = 0.5
    quick_heads = jax.random.uniform(pick_key, (HEADS,), jnp.float32) < share
    slow_rate = jnp.exp(jax.random.uniform(slow_key, (HEADS,), jnp.float32, jnp.log(0.2), jnp.log(0.8))) / SEQ
    quick_rate = jnp.exp(jax.random.uniform(quick_key, (HEADS,), jnp.float32, jnp.log(0.02), jnp.log(0.06)))
    return jnp.where(quick_heads, quick_rate, slow_rate)


def draw_rates(key, part):
    return rate_table(key).astype(jnp.float32)


def draw_decay_in(key, part):
    attender_forgetting_speed = rate_table(key)
    own = jax.random.fold_in(key, 202)
    factor_key, each_key, spot_key, loss_key = jax.random.split(own, 4)
    block_count = SEQ // TOK_DEV
    partition_multiplier = jnp.exp(jax.random.uniform(factor_key, (SEQS, block_count, 1, 1), jnp.float32, jnp.log(0.5), jnp.log(2.0)))
    each = jnp.exp(jax.random.uniform(each_key, (SEQS, block_count, TOK_DEV, HEADS), jnp.float32, jnp.log(0.7), jnp.log(1.4)))
    overall_item_count = (partition_multiplier * each).reshape(SEQS, SEQ, HEADS)
    spots = jax.random.randint(spot_key, (SEQS, 3), 0, SEQ)
    objective_figures = jax.random.uniform(loss_key, (SEQS, 3, HEADS), jnp.float32, 0.22, 0.4)
    discarded_items = (jnp.arange(SEQ)[None, :, None] == spots[:, None, :]).astype(jnp.float32)
    send_batch_count = jnp.einsum('mxb,mbn->mxn', discarded_items, objective_figures) / attender_forgetting_speed[None, None, :]
    overall_item_count = jnp.where(jnp.sum(discarded_items, axis=-1)[..., None] > 0.5, send_batch_count, overall_item_count)
    return (overall_item_count + jnp.log(-jnp.expm1(-overall_item_count))).astype(jnp.bfloat16)


def levels(own_key, shape, cuts, smallest, largest):
    loudness = 1.0
    for axis_at, parts in cuts:
        heights = jax.random.uniform(jax.random.fold_in(jax.random.fold_in(own_key, 6), axis_at), (parts,), jnp.float32, smallest / len(cuts), largest / len(cuts))
        loudness = loudness * jnp.repeat(jnp.exp(heights), shape[axis_at] // parts).reshape((-1,) + (1,) * (len(shape) - 1 - axis_at))
    return loudness


def shared_out(rng, own, number, rows, number_of, top, bound, lean):
    sequence = jax.random.permutation(rng, number_of)
    crowded, common = load_shares(number_of, rows * top, bound, lean, True), load_shares(number_of, rows * top, bound, lean, False)
    places = jnp.arange(number_of)

    def named(sizes, turn):
        used = int((sizes > 0).sum())
        fixed = max(1, used // 4)
        moved = fixed + (places - fixed + turn * (used - fixed)) % max(1, number_of - fixed)
        return jnp.zeros((number_of,), jnp.int32).at[sequence[jnp.where(places < fixed, places, moved)]].set(jnp.asarray(sizes, jnp.int32))

    sizes = jnp.where(number % 4 == 0, named(crowded, number // 4), named(common, number - number // 4 - 1))
    mixed = jax.random.permutation(jax.random.fold_in(own, 3), number_of)
    giver, taker = mixed[0:number_of // 2 * 2:2], mixed[1:number_of // 2 * 2:2]
    room = jnp.minimum(sizes[giver] - 1, bound - sizes[taker]) // 2
    room = jnp.where((giver == sequence[0]) | (taker == sequence[0]) | (sizes[taker] == 0), 0, jnp.maximum(room, 0))
    moved = jax.random.randint(jax.random.fold_in(own, 4), (number_of // 2,), 0, 1 << 20) % (room + 1)
    sizes = sizes.at[giver].add(-moved).at[taker].add(moved)
    labels = jnp.searchsorted(jnp.cumsum(sizes), jnp.arange(rows * top), side="right").astype(jnp.int32)
    listing = labels.reshape(top, rows).T
    listing = listing[jax.random.permutation(jax.random.fold_in(own, 1), rows)]
    turn = jax.random.randint(jax.random.fold_in(own, 2), (rows, 1), 0, top)
    return jnp.take_along_axis(listing, (jnp.arange(top)[None, :] + turn) % top, axis=1)


def load_shares(amount, total, limit, skew, full):
    loads = [(1 << 20) // math.isqrt(rank ** skew) + 1 for rank in range(1, amount + 1)]
    largest = limit if full else min(limit, max(-(-total // amount), total * loads[0] // sum(loads)))
    least = 1 if total - largest >= amount - 1 else 0
    counts, surplus = [largest] + [least] * (amount - 1), total - largest - least * (amount - 1)
    while surplus > 0:
        movable = [i for i in range(1, amount) if counts[i] < largest] or [i for i in range(1, amount) if counts[i] < limit]
        mass, left = sum([loads[i] for i in movable]), surplus
        for i in movable:
            extra = min(limit - counts[i], max(1, left * loads[i] // mass), surplus)
            counts[i] = counts[i] + extra
            surplus = surplus - extra
    return np.array(counts)


def normal_values(key, dims, scale, limit, cuts=(), kind=jnp.bfloat16):
    entries = jax.random.normal(key, dims, jnp.float32) * scale
    if len(cuts) > 0:
        entries = levels(key, dims, cuts, -0.22, 0.18) * entries
    return jnp.clip(entries, min=-limit, max=limit).astype(kind)


def setup_inputs(seed: int = 0) -> dict:
    streams_of = jax.random.split(jax.random.key(seed), 18)
    queries = normal_values(streams_of[0], (SEQS, SEQ, HEADS * DK), 1.0, 6.0, ((0, 4), (1, 8)))
    keys = normal_values(streams_of[1], (SEQS, SEQ, HEADS * DK), 1.0, 6.0, ((0, 4), (1, 8)))
    values = normal_values(streams_of[2], (SEQS, SEQ, HEADS * DV), 1.0, 6.0, ((0, 4), (1, 8)))
    decay_in = draw_decay_in(jax.random.fold_in(streams_of[17], 71), 0)
    mix_in = normal_values(streams_of[4], (SEQS, SEQ, HEADS), 1.5, 6.0, ((0, 4), (1, 8)))
    rates = draw_rates(jax.random.fold_in(streams_of[17], 71), 0)
    head_gain = jnp.clip(1.0 + 0.18 * jax.random.normal(streams_of[6], (DV,), jnp.float32), 0.1, 1.9)
    out_weight = normal_values(streams_of[7], (HEADS * DV, D), (HEADS * DV) ** -0.5, 0.125)
    residual = normal_values(streams_of[8], (SEQS, SEQ, D), 1.0, 6.0, ((0, 4), (1, 8)))
    mix_gain = jnp.clip(1.0 + 0.18 * jax.random.normal(streams_of[9], (D,), jnp.float32), 0.1, 1.9)
    ffn_gain = jnp.clip(1.0 + 0.18 * jax.random.normal(streams_of[10], (D,), jnp.float32), 0.1, 1.9)
    route_keys = jax.random.split(jax.random.fold_in(streams_of[11], 1), SEQS * SEQ // TOK_DEV)
    route_turns = jax.random.permutation(jax.random.fold_in(streams_of[11], 3), SEQS * SEQ // TOK_DEV)
    route = jax.vmap(lambda own, number: shared_out(jax.random.fold_in(streams_of[11], 2), own, number, TOK_DEV, EXPERTS, TOPK, CAP, 1))(route_keys, route_turns).reshape((SEQS, SEQ, TOPK))
    route_weight = jnp.clip(0.1 + 0.9 * jax.random.uniform(streams_of[12], (SEQS, SEQ, TOPK), jnp.float32) ** levels(streams_of[12], (SEQS, SEQ, TOPK), ((0, 4), (1, 8)), -0.2, 0.2), 0.1, 1.0)
    w_gate = normal_values(streams_of[13], (EXPERTS, D, FF), D ** -0.5, 0.125, ((0, 32),))
    w_up = normal_values(streams_of[14], (EXPERTS, D, FF), D ** -0.5, 0.125, ((0, 32),))
    w_down = normal_values(streams_of[15], (EXPERTS, FF, D), FF ** -0.5, 0.25, ((0, 32),))
    out_gain = jnp.clip(1.0 + 0.18 * jax.random.normal(streams_of[16], (D,), jnp.float32), 0.1, 1.9)
    return dict(queries=queries, keys=keys, values=values, decay_in=decay_in, mix_in=mix_in, rates=rates, head_gain=head_gain, out_weight=out_weight, residual=residual, mix_gain=mix_gain, ffn_gain=ffn_gain, route=route, route_weight=route_weight, w_gate=w_gate, w_up=w_up, w_down=w_down, out_gain=out_gain)


EPSILON = 1e-06
PRECISE = lax.Precision.HIGHEST

def unit_rows(weight_matrix):
    return weight_matrix * lax.rsqrt(lax.optimization_barrier(jnp.sum(weight_matrix * weight_matrix, axis=-1, keepdims=True)) + EPSILON)

def scale_rows(weight_matrix, gain):
    return weight_matrix * lax.rsqrt(lax.optimization_barrier(jnp.mean(weight_matrix * weight_matrix, axis=-1, keepdims=True)) + EPSILON) * gain

def unit_lower_inverse(strict_part):
    identity = jnp.eye(strict_part.shape[-1], dtype=jnp.float32)
    power_term = -strict_part
    result = identity + power_term
    for section_index in range(strict_part.shape[-1].bit_length() - 2):
        power_term = jnp.matmul(power_term, power_term, precision=PRECISE)
        result = result + jnp.matmul(result, power_term, precision=PRECISE)
    return result

def carry_block(state, inputs_now):
    query_now, key_now, update_now, correct_now, score_now, total_now = inputs_now
    fresh = update_now - jnp.einsum('hcd,hde->hce', correct_now, state, precision=PRECISE)
    output = jnp.einsum('hcd,hde->hce', query_now, state, precision=PRECISE)
    output = output + jnp.einsum('hcs,hse->hce', score_now, fresh, precision=PRECISE)
    state = state * total_now[:, None, None] + jnp.einsum('hcd,hce->hde', key_now, fresh, precision=PRECISE)
    return (state, output)

def delta_rule(unit_query, unit_key, value_rows, log_decay, mixing):
    head_count, length, key_width = unit_query.shape
    value_width = value_rows.shape[-1]
    block_count = length // BLOCK

    def tiles(weight_matrix):
        return weight_matrix.reshape((head_count, block_count, BLOCK) + weight_matrix.shape[2:])
    query_half = tiles(unit_query).astype(jnp.float32)
    key_half = tiles(unit_key).astype(jnp.float32)
    query_tiles = query_half * key_width ** (-0.5)
    key_tiles = key_half
    value_tiles = tiles(value_rows)
    beta_tiles = tiles(mixing)
    running = jnp.cumsum(tiles(log_decay), axis=-1)
    offsets = jnp.arange(BLOCK, dtype=jnp.int32)
    lower_mask = offsets[:, None] >= offsets[None, :]
    strict_mask = offsets[:, None] > offsets[None, :]
    spread = running[..., :, None] - running[..., None, :]
    decay_tiles = jnp.where(lower_mask, jnp.exp(jnp.where(lower_mask, spread, 0.0)), 0.0)
    key_beta = key_tiles * beta_tiles[..., None]
    key_pairs = jnp.einsum('hncd,hnsd->hncs', key_half, key_half, precision=PRECISE)
    strict_part = jnp.where(strict_mask, key_pairs * beta_tiles[..., None] * decay_tiles, 0.0)
    inverse = unit_lower_inverse(strict_part)
    update = jnp.einsum('hncs,hnse->hnce', inverse, value_tiles * beta_tiles[..., None], precision=PRECISE)
    correction = jnp.einsum('hncs,hnsd->hncd', inverse, key_beta * jnp.exp(running)[..., None], precision=PRECISE)
    query_pairs = jnp.einsum('hncd,hnsd->hncs', query_half, key_half, precision=PRECISE)
    scores = query_pairs * key_width ** (-0.5) * decay_tiles
    query_decay = query_tiles * jnp.exp(running)[..., None]
    key_decay = key_tiles * jnp.exp(running[..., -1:] - running)[..., None]
    total_decay = jnp.exp(running[..., -1])
    sequence_in = tuple((jnp.moveaxis(group_member, 1, 0) for group_member in (query_decay, key_decay, update, correction, scores, total_decay)))
    initial = jnp.zeros((head_count, key_width, value_width), jnp.float32)
    final_state, outputs = lax.scan(carry_block, initial, sequence_in)
    return jnp.transpose(outputs, (1, 0, 2, 3)).reshape(head_count, length, value_width)

def attend(query_heads, key_heads, value_heads, decay_heads, mix_heads, decay_scales, head_gain):
    unit_query = unit_rows(query_heads.astype(jnp.float32)).astype(jnp.bfloat16)
    unit_key = unit_rows(key_heads.astype(jnp.float32)).astype(jnp.bfloat16)
    log_decay = -decay_scales[:, None] * jax.nn.softplus(decay_heads.astype(jnp.float32))
    mixing = jax.nn.sigmoid(mix_heads.astype(jnp.float32))
    output = delta_rule(unit_query, unit_key, value_heads.astype(jnp.float32), log_decay, mixing)
    return scale_rows(output, head_gain).astype(jnp.bfloat16)

def expert_ffn(rows_in, gate_weight, up_weight, down_weight):
    gate = jnp.dot(rows_in, gate_weight, preferred_element_type=jnp.float32)
    upward = jnp.dot(rows_in, up_weight, preferred_element_type=jnp.float32)
    inner = (jax.nn.silu(gate) * upward).astype(jnp.bfloat16)
    return jnp.dot(inner, down_weight, preferred_element_type=jnp.float32).astype(jnp.bfloat16)

def reference(queries, keys, values, decay_in, mix_in, rates, head_gain, out_weight, residual, mix_gain, ffn_gain, route, route_weight, w_gate, w_up, w_down, out_gain):

    def heads_first(weight_matrix, width):
        return weight_matrix.reshape(SEQ, HEADS, width).transpose(1, 0, 2)

    def one_sequence(pieces):
        question_series, key_seq, value_seq, decay_seq, mix_seq = pieces
        output = attend(heads_first(question_series, DK), heads_first(key_seq, DK), heads_first(value_seq, DV), decay_seq.T, mix_seq.T, rates, head_gain)
        return output.transpose(1, 0, 2).reshape(SEQ, HEADS * DV)
    attended = lax.map(one_sequence, (queries, keys, values, decay_in, mix_in))
    tokens = SEQS * SEQ
    attended = attended.reshape(tokens, HEADS * DV)
    projected = jnp.dot(attended, out_weight, preferred_element_type=jnp.float32)
    hidden_state = (residual.reshape(tokens, D).astype(jnp.float32) + scale_rows(projected, mix_gain)).astype(jnp.bfloat16)
    normed = scale_rows(hidden_state.astype(jnp.float32), ffn_gain).astype(jnp.bfloat16)
    blocks = tokens // TOK_DEV
    route_ids = route.reshape(blocks, TOK_DEV * TOPK)
    matches = (route_ids[..., None] == jnp.arange(EXPERTS, dtype=jnp.int32)).astype(jnp.int32)
    slot_index = lax.optimization_barrier(jnp.sum((jnp.cumsum(matches, axis=1) - 1) * matches, axis=-1))
    expert_of = route_ids.reshape(-1)
    owners = jnp.arange(tokens * TOPK, dtype=jnp.int32) // TOPK
    columns = (jnp.arange(blocks, dtype=jnp.int32)[:, None] * CAP + slot_index).reshape(-1)
    sources = jnp.zeros((EXPERTS, blocks * CAP), jnp.int32).at[expert_of, columns].set(owners)
    weights = jnp.zeros((EXPERTS, blocks * CAP), jnp.float32).at[expert_of, columns].set(route_weight.reshape(-1))

    def append_specialist(total, pieces):
        source_rows, source_weights, gate_weight, up_weight, down_weight = pieces
        output = expert_ffn(normed[source_rows], gate_weight, up_weight, down_weight)
        return (total.at[source_rows].add(source_weights[:, None] * output.astype(jnp.float32)), None)
    combined, unused = lax.scan(append_specialist, jnp.zeros((tokens, D), jnp.float32), (sources, weights, w_gate, w_up, w_down))
    mixed = (hidden_state.astype(jnp.float32) + scale_rows(combined, out_gain)).astype(jnp.bfloat16)
    return mixed.reshape(SEQS, SEQ, D)
```

```python
import functools

import jax
import jax.numpy as jnp
from jax import lax
from jax.experimental import pallas as pl
from jax.experimental.pallas import tpu as pltpu
from jax.sharding import PartitionSpec as P

DK = 64
DV = 128
TOPK = 2
BLOCK = 128
EPSILON = 1e-06
PRECISE = lax.Precision.HIGHEST
MESH = pl.DeviceIdType.MESH
VMEM = pl.BlockSpec(memory_space=pltpu.VMEM)
ANY = pl.BlockSpec(memory_space=pl.ANY)
HALF = jnp.bfloat16
NN = (((1,), (0,)), ((), ()))
NT = (((1,), (1,)), ((), ()))
TN = (((0,), (0,)), ((), ()))


def dot(a, b, dims=NN, precision=None):
    return lax.dot_general(a, b, dims, precision=precision, preferred_element_type=jnp.float32)


def unit_rows(x):
    return x * lax.rsqrt(jnp.sum(x * x, axis=-1, keepdims=True) + EPSILON)


def scale_rows(x, gain):
    return x * lax.rsqrt(jnp.mean(x * x, axis=-1, keepdims=True) + EPSILON) * gain


def pair_width(local_heads):
    return max(DV, local_heads * DK)


def block_kernel(groups, local_heads, q_ref, k_ref, v_ref, decay_ref, mix_ref, rates_ref, ab_ref, o_ref, qe_ref):
    length = q_ref.shape[0]
    heads = groups * local_heads
    rows = lax.broadcasted_iota(jnp.int32, (length, length), 0)
    cols = lax.broadcasted_iota(jnp.int32, (length, length), 1)
    lower = rows >= cols
    strict = rows > cols
    decay = decay_ref[...].astype(jnp.float32)
    softplus = jnp.maximum(decay, 0.0) + jnp.log1p(jnp.exp(-jnp.abs(decay)))
    log_decay = -rates_ref[...] * softplus
    beta = 1.0 / (1.0 + jnp.exp(-mix_ref[...].astype(jnp.float32)))
    running = dot(lower.astype(jnp.float32), log_decay, NN, PRECISE)
    spot_r = lax.broadcasted_iota(jnp.int32, (heads, heads), 0)
    spot_c = lax.broadcasted_iota(jnp.int32, (heads, heads), 1)
    running_t = dot((spot_r == spot_c).astype(jnp.float32), running, NT, PRECISE)
    grow = jnp.exp(running)
    total = running[length - 1 : length, :]
    shrink = jnp.exp(total - running)
    whole = jnp.exp(total)
    eye = (
        lax.broadcasted_iota(jnp.int32, (DK, DK), 0) == lax.broadcasted_iota(jnp.int32, (DK, DK), 1)
    ).astype(jnp.float32)
    scale = DK ** (-0.5)
    batch = 8 if heads % 8 == 0 else 1
    base = pair_width(local_heads)
    for first in range(0, heads, batch):
        own = range(first, first + batch)
        work = []
        for h in own:
            qn = unit_rows(q_ref[:, h * DK : (h + 1) * DK].astype(jnp.float32)).astype(HALF)
            kn = unit_rows(k_ref[:, h * DK : (h + 1) * DK].astype(jnp.float32)).astype(HALF)
            spread = running[:, h : h + 1] - running_t[h : h + 1, :]
            tile = jnp.where(lower, jnp.exp(jnp.where(lower, spread, 0.0)), 0.0)
            bet = beta[:, h : h + 1]
            strict_part = jnp.where(strict, dot(kn, kn, NT) * bet * tile, 0.0)
            scores = (dot(qn, kn, NT) * scale * tile).astype(HALF)
            work.append((qn, kn, strict_part, scores))
        size = 1
        inverses = [None] * batch
        while size < length:
            joins = (rows // (2 * size) == cols // (2 * size)) & ((rows // size) % 2 == 1) & ((cols // size) % 2 == 0)
            for i in range(batch):
                part = jnp.where(joins, work[i][2], 0.0)
                if size == 1:
                    inverses[i] = (rows == cols).astype(jnp.float32) - part
                else:
                    half = inverses[i].astype(HALF)
                    step = dot(part.astype(HALF), half)
                    inverses[i] = inverses[i] - dot(half, step.astype(HALF))
            size *= 2
        for i, h in enumerate(own):
            qn, kn, strict_part, scores = work[i]
            bet = beta[:, h : h + 1]
            key = kn.astype(jnp.float32)
            values = v_ref[:, h * DV : (h + 1) * DV].astype(jnp.float32) * bet
            inputs = jnp.concatenate([values, key * (bet * grow[:, h : h + 1])], axis=1)
            solved = dot(inverses[i].astype(HALF), inputs.astype(HALF))
            solved = solved.astype(HALF)
            seen = dot(scores, solved)
            kept = dot((key * shrink[:, h : h + 1]).astype(HALF), solved, TN)
            o_ref[:, h * DV : (h + 1) * DV] = seen[:, :DV]
            query = qn.astype(jnp.float32) * (scale * grow[:, h : h + 1])
            qe_ref[h] = (query - seen[:, DV:]).astype(HALF)
            owner, place = h // local_heads, h % local_heads
            ab_ref[owner, :, base + place * DV : base + (place + 1) * DV] = kept[:, :DV].astype(HALF)
            ab_ref[owner, :, place * DK : (place + 1) * DK] = (
                eye * whole[:, h : h + 1] - kept[:, DV:]
            ).astype(HALF)
            if local_heads * DK < base and place == local_heads - 1:
                ab_ref[owner, :, local_heads * DK : base] = jnp.zeros((DK, base - local_heads * DK), HALF)


def state_kernel(
    groups, local_heads,
    ab_ref, o_ref, qe_ref, hg_ref, w_hbm, res_ref, mg_ref, fg_ref,
    hidden_ref, normed_ref,
    ab_in, s_out, s_in, att, w_ref,
    w_sem, own_sem, send1, recv1, send2, recv2,
):
    me = lax.axis_index("sp")
    fetch = pltpu.make_async_copy(w_hbm, w_ref, w_sem)
    fetch.start()
    barrier = pltpu.get_barrier_semaphore()
    for step in range(1, groups):
        pl.semaphore_signal(barrier, inc=1, device_id={"sp": lax.rem(me + step, groups)}, device_id_type=MESH)
    pl.semaphore_wait(barrier, groups - 1)

    def first_copy(step):
        peer = lax.rem(me + step, groups)
        return pltpu.make_async_remote_copy(
            src_ref=ab_ref.at[peer], dst_ref=ab_in.at[me],
            send_sem=send1.at[step], recv_sem=recv1.at[step],
            device_id={"sp": peer}, device_id_type=MESH,
        )

    def second_copy(step):
        peer = lax.rem(me + step, groups)
        return pltpu.make_async_remote_copy(
            src_ref=s_out.at[peer], dst_ref=s_in.at[me],
            send_sem=send2.at[step], recv_sem=recv2.at[step],
            device_id={"sp": peer}, device_id_type=MESH,
        )

    for step in range(1, groups):
        first_copy(step).start()
    own = pltpu.make_async_copy(ab_ref.at[me], ab_in.at[me], own_sem)
    own.start()
    own.wait()
    for step in range(1, groups):
        first_copy(step).wait()
    base = pair_width(local_heads)
    states = [jnp.zeros((DK, DV), jnp.float32)] * local_heads
    for block in range(groups):
        for place in range(local_heads):
            half = states[place].astype(HALF)
            s_out[block, :, place * DV : (place + 1) * DV] = half
            if block < groups - 1:
                states[place] = (
                    dot(ab_in[block, :, place * DK : (place + 1) * DK], half)
                    + ab_in[block, :, base + place * DV : base + (place + 1) * DV].astype(jnp.float32)
                )
    for step in range(1, groups):
        second_copy(step).start()
    own = pltpu.make_async_copy(s_out.at[me], s_in.at[me], own_sem)
    own.start()
    own.wait()
    for step in range(1, groups):
        second_copy(step).wait()
    for h in range(groups * local_heads):
        owner, place = h // local_heads, h % local_heads
        state = s_in[owner, :, place * DV : (place + 1) * DV]
        out = o_ref[:, h * DV : (h + 1) * DV] + dot(qe_ref[h], state)
        att[:, h * DV : (h + 1) * DV] = scale_rows(out, hg_ref[...]).astype(HALF)
    fetch.wait()
    projected = dot(att[...], w_ref[...])
    hidden = (res_ref[...].astype(jnp.float32) + scale_rows(projected, mg_ref[...])).astype(HALF)
    hidden_ref[...] = hidden
    normed_ref[...] = scale_rows(hidden.astype(jnp.float32), fg_ref[...]).astype(HALF)


def expert_ffn(rows_in, gate_weight, up_weight, down_weight):
    gate = jnp.dot(rows_in, gate_weight, preferred_element_type=jnp.float32)
    upward = jnp.dot(rows_in, up_weight, preferred_element_type=jnp.float32)
    inner = (jax.nn.silu(gate) * upward).astype(jnp.bfloat16)
    return jnp.dot(inner, down_weight, preferred_element_type=jnp.float32).astype(jnp.bfloat16)


def local(
    queries,
    keys,
    values,
    decay_in,
    mix_in,
    rates,
    head_gain,
    out_weight,
    residual,
    mix_gain,
    ffn_gain,
    route,
    route_weight,
    w_gate,
    w_up,
    w_down,
    out_gain,
):
    groups = lax.axis_size("sp")
    tok_rows = queries.shape[1]
    head_count = rates.shape[0]
    local_heads = head_count // groups
    width = out_weight.shape[1]
    wide = pair_width(local_heads) + local_heads * DV
    pairs, partial, reads = pl.pallas_call(
        functools.partial(block_kernel, groups, local_heads),
        out_shape=(
            jax.ShapeDtypeStruct((groups, DK, wide), HALF),
            jax.ShapeDtypeStruct((tok_rows, head_count * DV), jnp.float32),
            jax.ShapeDtypeStruct((head_count, tok_rows, DK), HALF),
        ),
        in_specs=[VMEM] * 6,
        out_specs=(VMEM,) * 3,
        compiler_params=pltpu.CompilerParams(vmem_limit_bytes=40 << 20),
        name="block",
    )(queries[0], keys[0], values[0], decay_in[0], mix_in[0], rates.reshape(1, head_count))
    hidden_state, normed = pl.pallas_call(
        functools.partial(state_kernel, groups, local_heads),
        out_shape=(jax.ShapeDtypeStruct((tok_rows, width), HALF),) * 2,
        in_specs=[VMEM] * 4 + [ANY] + [VMEM] * 3,
        out_specs=(VMEM,) * 2,
        scratch_shapes=[
            pltpu.VMEM((groups, DK, wide), HALF),
            pltpu.VMEM((groups, DK, local_heads * DV), HALF),
            pltpu.VMEM((groups, DK, local_heads * DV), HALF),
            pltpu.VMEM((tok_rows, head_count * DV), HALF),
            pltpu.VMEM(out_weight.shape, HALF),
            pltpu.SemaphoreType.DMA,
            pltpu.SemaphoreType.DMA,
        ]
        + [pltpu.SemaphoreType.DMA((groups,))] * 4,
        compiler_params=pltpu.CompilerParams(
            collective_id=0, has_side_effects=True, vmem_limit_bytes=40 << 20
        ),
        name="state",
    )(
        pairs, partial, reads, head_gain.reshape(1, DV), out_weight, residual[0],
        mix_gain.reshape(1, width), ffn_gain.reshape(1, width),
    )
    experts = lax.axis_size("sp") * lax.axis_size("dp")
    capacity = max(2, 2 * tok_rows * TOPK // experts)
    route_ids = route.reshape(tok_rows * TOPK)
    matches = (route_ids[:, None] == jnp.arange(experts, dtype=jnp.int32)).astype(jnp.int32)
    slot_index = jnp.sum((jnp.cumsum(matches, axis=0) - 1) * matches, axis=-1)
    target = route_ids * capacity + slot_index
    copies = jnp.repeat(normed, TOPK, axis=0)
    outgoing = jnp.zeros((experts * capacity, width), jnp.bfloat16).at[target].set(copies)
    arrived_block = lax.all_to_all(
        outgoing.reshape(experts, capacity, width),
        ("sp", "dp"),
        split_axis=0,
        concat_axis=0,
        tiled=True,
    )
    block_shape = arrived_block.shape
    flat_rows = arrived_block.reshape(-1, block_shape[-1])
    served = expert_ffn(flat_rows, w_gate[0], w_up[0], w_down[0]).reshape(block_shape)
    returned = lax.all_to_all(served, ("sp", "dp"), split_axis=0, concat_axis=0, tiled=True)
    gathered = returned.reshape(experts * capacity, width)[target].reshape(tok_rows, TOPK, width)
    combined = jnp.sum(
        route_weight.reshape(tok_rows, TOPK, 1) * gathered.astype(jnp.float32), axis=1
    )
    mixed = (hidden_state.astype(jnp.float32) + scale_rows(combined, out_gain)).astype(jnp.bfloat16)
    return mixed.reshape(1, tok_rows, width)


def solution(mesh):
    in_specs = (
        P("dp", "sp", None),
        P("dp", "sp", None),
        P("dp", "sp", None),
        P("dp", "sp", None),
        P("dp", "sp", None),
        P(),
        P(),
        P(),
        P("dp", "sp", None),
        P(),
        P(),
        P("dp", "sp", None),
        P("dp", "sp", None),
        P(("sp", "dp"), None, None),
        P(("sp", "dp"), None, None),
        P(("sp", "dp"), None, None),
        P(),
    )
    out_specs = P("dp", "sp", None)
    return jax.shard_map(local, mesh=mesh, in_specs=in_specs, out_specs=out_specs, check_vma=False)
```

```python
import functools

import jax
import jax.numpy as jnp
from jax import lax
from jax.experimental import pallas as pl
from jax.experimental.pallas import tpu as pltpu
from jax.sharding import PartitionSpec as P

DK = 64
DV = 128
TOPK = 2
BLOCK = 128
EPSILON = 1e-06
PRECISE = lax.Precision.HIGHEST
MESH = pl.DeviceIdType.MESH
VMEM = pl.BlockSpec(memory_space=pltpu.VMEM)
ANY = pl.BlockSpec(memory_space=pl.ANY)
HALF = jnp.bfloat16
NN = (((1,), (0,)), ((), ()))
NT = (((1,), (1,)), ((), ()))
TN = (((0,), (0,)), ((), ()))


def dot(a, b, dims=NN, precision=None):
    return lax.dot_general(a, b, dims, precision=precision, preferred_element_type=jnp.float32)


def unit_rows(x):
    return x * lax.rsqrt(jnp.sum(x * x, axis=-1, keepdims=True) + EPSILON)


def scale_rows(x, gain):
    return x * lax.rsqrt(jnp.mean(x * x, axis=-1, keepdims=True) + EPSILON) * gain


def pair_width(local_heads):
    return max(DV, local_heads * DK)


def block_kernel(groups, local_heads, q_ref, k_ref, v_ref, decay_ref, mix_ref, rates_ref, ab_ref, o_ref, qe_ref):
    length = q_ref.shape[0]
    heads = groups * local_heads
    rows = lax.broadcasted_iota(jnp.int32, (length, length), 0)
    cols = lax.broadcasted_iota(jnp.int32, (length, length), 1)
    lower = rows >= cols
    strict = rows > cols
    decay = decay_ref[...].astype(jnp.float32)
    softplus = jnp.maximum(decay, 0.0) + jnp.log1p(jnp.exp(-jnp.abs(decay)))
    log_decay = -rates_ref[...] * softplus
    beta = 1.0 / (1.0 + jnp.exp(-mix_ref[...].astype(jnp.float32)))
    running = dot(lower.astype(jnp.float32), log_decay, NN, PRECISE)
    spot_r = lax.broadcasted_iota(jnp.int32, (heads, heads), 0)
    spot_c = lax.broadcasted_iota(jnp.int32, (heads, heads), 1)
    running_t = dot((spot_r == spot_c).astype(jnp.float32), running, NT, PRECISE)
    grow = jnp.exp(running)
    total = running[length - 1 : length, :]
    shrink = jnp.exp(total - running)
    whole = jnp.exp(total)
    eye = (
        lax.broadcasted_iota(jnp.int32, (DK, DK), 0) == lax.broadcasted_iota(jnp.int32, (DK, DK), 1)
    ).astype(jnp.float32)
    scale = DK ** (-0.5)
    batch = 8 if heads % 8 == 0 else 1
    base = pair_width(local_heads)
    for first in range(0, heads, batch):
        own = range(first, first + batch)
        work = []
        for h in own:
            qn = unit_rows(q_ref[:, h * DK : (h + 1) * DK].astype(jnp.float32)).astype(HALF)
            kn = unit_rows(k_ref[:, h * DK : (h + 1) * DK].astype(jnp.float32)).astype(HALF)
            spread = running[:, h : h + 1] - running_t[h : h + 1, :]
            tile = jnp.where(lower, jnp.exp(jnp.where(lower, spread, 0.0)), 0.0)
            bet = beta[:, h : h + 1]
            strict_part = jnp.where(strict, dot(kn, kn, NT) * bet * tile, 0.0)
            scores = (dot(qn, kn, NT) * scale * tile).astype(HALF)
            work.append((qn, kn, strict_part, scores))
        size = 1
        inverses = [None] * batch
        while size < length:
            joins = (rows // (2 * size) == cols // (2 * size)) & ((rows // size) % 2 == 1) & ((cols // size) % 2 == 0)
            for i in range(batch):
                part = jnp.where(joins, work[i][2], 0.0)
                if size == 1:
                    inverses[i] = (rows == cols).astype(jnp.float32) - part
                else:
                    half = inverses[i].astype(HALF)
                    step = dot(part.astype(HALF), half)
                    inverses[i] = inverses[i] - dot(half, step.astype(HALF))
            size *= 2
        for i, h in enumerate(own):
            qn, kn, strict_part, scores = work[i]
            bet = beta[:, h : h + 1]
            key = kn.astype(jnp.float32)
            values = v_ref[:, h * DV : (h + 1) * DV].astype(jnp.float32) * bet
            inputs = jnp.concatenate([values, key * (bet * grow[:, h : h + 1])], axis=1)
            solved = dot(inverses[i].astype(HALF), inputs.astype(HALF))
            solved = solved.astype(HALF)
            seen = dot(scores, solved)
            kept = dot((key * shrink[:, h : h + 1]).astype(HALF), solved, TN)
            o_ref[:, h * DV : (h + 1) * DV] = seen[:, :DV]
            query = qn.astype(jnp.float32) * (scale * grow[:, h : h + 1])
            qe_ref[h] = (query - seen[:, DV:]).astype(HALF)
            owner, place = h // local_heads, h % local_heads
            ab_ref[owner, :, base + place * DV : base + (place + 1) * DV] = kept[:, :DV].astype(HALF)
            ab_ref[owner, :, place * DK : (place + 1) * DK] = (
                eye * whole[:, h : h + 1] - kept[:, DV:]
            ).astype(HALF)
            if local_heads * DK < base and place == local_heads - 1:
                ab_ref[owner, :, local_heads * DK : base] = jnp.zeros((DK, base - local_heads * DK), HALF)


def state_kernel(
    groups, local_heads,
    ab_ref, o_ref, qe_ref, hg_ref, w_hbm, res_ref, mg_ref, fg_ref,
    hidden_ref, normed_ref,
    ab_in, s_out, s_in, att, w_ref,
    w_sem, own_sem, send1, recv1, send2, recv2,
):
    me = lax.axis_index("sp")
    fetch = pltpu.make_async_copy(w_hbm, w_ref, w_sem)
    fetch.start()
    barrier = pltpu.get_barrier_semaphore()
    for step in range(1, groups):
        pl.semaphore_signal(barrier, inc=1, device_id={"sp": lax.rem(me + step, groups)}, device_id_type=MESH)
    pl.semaphore_wait(barrier, groups - 1)

    def first_copy(step):
        peer = lax.rem(me + step, groups)
        return pltpu.make_async_remote_copy(
            src_ref=ab_ref.at[peer], dst_ref=ab_in.at[me],
            send_sem=send1.at[step], recv_sem=recv1.at[step],
            device_id={"sp": peer}, device_id_type=MESH,
        )

    def second_copy(step):
        peer = lax.rem(me + step, groups)
        return pltpu.make_async_remote_copy(
            src_ref=s_out.at[peer], dst_ref=s_in.at[me],
            send_sem=send2.at[step], recv_sem=recv2.at[step],
            device_id={"sp": peer}, device_id_type=MESH,
        )

    for step in range(1, groups):
        first_copy(step).start()
    own = pltpu.make_async_copy(ab_ref.at[me], ab_in.at[me], own_sem)
    own.start()
    own.wait()
    for step in range(1, groups):
        first_copy(step).wait()
    base = pair_width(local_heads)
    states = [jnp.zeros((DK, DV), jnp.float32)] * local_heads
    for block in range(groups):
        for place in range(local_heads):
            half = states[place].astype(HALF)
            s_out[block, :, place * DV : (place + 1) * DV] = half
            if block < groups - 1:
                states[place] = (
                    dot(ab_in[block, :, place * DK : (place + 1) * DK], half)
                    + ab_in[block, :, base + place * DV : base + (place + 1) * DV].astype(jnp.float32)
                )
    for step in range(1, groups):
        second_copy(step).start()
    own = pltpu.make_async_copy(s_out.at[me], s_in.at[me], own_sem)
    own.start()
    own.wait()
    for step in range(1, groups):
        second_copy(step).wait()
    for h in range(groups * local_heads):
        owner, place = h // local_heads, h % local_heads
        state = s_in[owner, :, place * DV : (place + 1) * DV]
        out = o_ref[:, h * DV : (h + 1) * DV] + dot(qe_ref[h], state)
        att[:, h * DV : (h + 1) * DV] = scale_rows(out, hg_ref[...]).astype(HALF)
    fetch.wait()
    projected = dot(att[...], w_ref[...])
    hidden = (res_ref[...].astype(jnp.float32) + scale_rows(projected, mg_ref[...])).astype(HALF)
    hidden_ref[...] = hidden
    normed_ref[...] = scale_rows(hidden.astype(jnp.float32), fg_ref[...]).astype(HALF)


def flip(index, mask, bits):
    result = 0
    for bit in range(bits):
        own = (index // (1 << bit)) % 2
        other = (mask // (1 << bit)) % 2
        result = result + (own + other - 2 * own * other) * (1 << bit)
    return result


def expert_kernel(
    groups, members, capacity,
    normed_ref, hidden_ref, route_ref, share_ref, gain_ref, gate_hbm, up_hbm, down_hbm,
    mixed_ref,
    outgoing, arrived, served, returned, gate_ref, up_ref, down_ref,
    w_sems, own_sem, send1, recv1, send2, recv2,
):
    sp, dp = lax.axis_index("sp"), lax.axis_index("dp")
    count = groups * members
    sp_bits, dp_bits = groups.bit_length() - 1, members.bit_length() - 1
    fetches = [
        pltpu.make_async_copy(source, target, w_sems.at[i])
        for i, (source, target) in enumerate(((gate_hbm, gate_ref), (up_hbm, up_ref), (down_hbm, down_ref)))
    ]
    for fetch in fetches:
        fetch.start()

    def masks(k):
        mask = count - 1 - k
        return mask // members, mask % members

    def partner(k):
        sp_mask, dp_mask = masks(k)
        return {"sp": flip(sp, sp_mask, sp_bits), "dp": flip(dp, dp_mask, dp_bits)}

    barrier = pltpu.get_barrier_semaphore()
    for k in range(count - 1):
        pl.semaphore_signal(barrier, inc=1, device_id=partner(k), device_id_type=MESH)

    tokens = normed_ref.shape[0]
    slots = count * capacity
    names = lax.broadcasted_iota(jnp.int32, (tokens, count), 1)
    first, second = route_ref[:, 0:1] == names, route_ref[:, 1:2] == names
    both = first.astype(jnp.float32) + second.astype(jnp.float32)
    rows = lax.broadcasted_iota(jnp.int32, (tokens, tokens), 0)
    cols = lax.broadcasted_iota(jnp.int32, (tokens, tokens), 1)
    before = dot((rows > cols).astype(HALF), both.astype(HALF))
    places = (both * (before + 1.0)).astype(HALF)
    share = first.astype(jnp.float32) * share_ref[:, 0:1] + second.astype(jnp.float32) * share_ref[:, 1:2]
    share_high = share.astype(HALF)
    share_low = (share - share_high.astype(jnp.float32)).astype(HALF)

    def owner_of(slot):
        sp_mask, dp_mask = masks(slot // capacity)
        return flip(sp, sp_mask, sp_bits) * members + flip(dp, dp_mask, dp_bits)

    down_slot = lax.broadcasted_iota(jnp.int32, (slots, count), 0)
    spread_rows = (owner_of(down_slot) == lax.broadcasted_iota(jnp.int32, (slots, count), 1)).astype(HALF)
    turn = (lax.broadcasted_iota(jnp.int32, (slots, tokens), 0) % capacity + 1).astype(jnp.float32)
    pick = (dot(spread_rows, places, NT) == turn).astype(HALF)
    normed = normed_ref[...]
    width = normed.shape[1]
    chunk = slots // 4 if slots % (4 * capacity) == 0 else slots
    per = chunk // capacity
    for at in range(0, slots, chunk):
        block = dot(pick[at : at + chunk], normed).astype(HALF)
        outgoing[at // capacity : at // capacity + per] = block.reshape(per, capacity, width)

    def go(k):
        return pltpu.make_async_remote_copy(
            src_ref=outgoing.at[k], dst_ref=arrived.at[k],
            send_sem=send1.at[k], recv_sem=recv1.at[k],
            device_id=partner(k), device_id_type=MESH,
        )

    def back(k):
        return pltpu.make_async_remote_copy(
            src_ref=served.at[k], dst_ref=returned.at[k],
            send_sem=send2.at[k], recv_sem=recv2.at[k],
            device_id=partner(k), device_id_type=MESH,
        )

    pl.semaphore_wait(barrier, count - 1)
    for k in range(count - 1):
        go(k).start()
    own = pltpu.make_async_copy(outgoing.at[count - 1], arrived.at[count - 1], own_sem)
    own.start()
    own.wait()
    match = dot(places, spread_rows, NT) == (
        lax.broadcasted_iota(jnp.int32, (tokens, slots), 1) % capacity + 1
    ).astype(jnp.float32)
    high = jnp.where(match, dot(share_high, spread_rows, NT), 0.0).astype(HALF)
    low = jnp.where(match, dot(share_low, spread_rows, NT), 0.0).astype(HALF)
    for fetch in fetches:
        fetch.wait()
    for at in range(0, count, per):
        for k in range(at, min(at + per, count - 1)):
            go(k).wait()
        rows_in = arrived[at : at + per].reshape(chunk, width)
        gate = dot(rows_in, gate_ref[...])
        inner = (gate / (1.0 + jnp.exp(-gate)) * dot(rows_in, up_ref[...])).astype(HALF)
        served[at : at + per] = dot(inner, down_ref[...]).astype(HALF).reshape(per, capacity, width)
        for k in range(at, min(at + per, count - 1)):
            back(k).start()
    own = pltpu.make_async_copy(served.at[count - 1], returned.at[count - 1], own_sem)
    own.start()
    own.wait()
    total = jnp.zeros((tokens, width), jnp.float32)
    for at in range(0, count, per):
        for k in range(at, min(at + per, count - 1)):
            back(k).wait()
        block = returned[at : at + per].reshape(chunk, width)
        low_slot, high_slot = at * capacity, at * capacity + chunk
        total = total + dot(high[:, low_slot:high_slot], block) + dot(low[:, low_slot:high_slot], block)
    mixed_ref[...] = (hidden_ref[...].astype(jnp.float32) + scale_rows(total, gain_ref[...])).astype(HALF)


def expert_ffn(rows_in, gate_weight, up_weight, down_weight):
    gate = jnp.dot(rows_in, gate_weight, preferred_element_type=jnp.float32)
    upward = jnp.dot(rows_in, up_weight, preferred_element_type=jnp.float32)
    inner = (jax.nn.silu(gate) * upward).astype(jnp.bfloat16)
    return jnp.dot(inner, down_weight, preferred_element_type=jnp.float32).astype(jnp.bfloat16)


def local(
    queries,
    keys,
    values,
    decay_in,
    mix_in,
    rates,
    head_gain,
    out_weight,
    residual,
    mix_gain,
    ffn_gain,
    route,
    route_weight,
    w_gate,
    w_up,
    w_down,
    out_gain,
):
    groups = lax.axis_size("sp")
    tok_rows = queries.shape[1]
    head_count = rates.shape[0]
    local_heads = head_count // groups
    width = out_weight.shape[1]
    wide = pair_width(local_heads) + local_heads * DV
    pairs, partial, reads = pl.pallas_call(
        functools.partial(block_kernel, groups, local_heads),
        out_shape=(
            jax.ShapeDtypeStruct((groups, DK, wide), HALF),
            jax.ShapeDtypeStruct((tok_rows, head_count * DV), jnp.float32),
            jax.ShapeDtypeStruct((head_count, tok_rows, DK), HALF),
        ),
        in_specs=[VMEM] * 6,
        out_specs=(VMEM,) * 3,
        compiler_params=pltpu.CompilerParams(vmem_limit_bytes=60 * 1024 * 1024),
        name="block",
    )(queries[0], keys[0], values[0], decay_in[0], mix_in[0], rates.reshape(1, head_count))
    hidden_state, normed = pl.pallas_call(
        functools.partial(state_kernel, groups, local_heads),
        out_shape=(jax.ShapeDtypeStruct((tok_rows, width), HALF),) * 2,
        in_specs=[VMEM] * 4 + [ANY] + [VMEM] * 3,
        out_specs=(VMEM,) * 2,
        scratch_shapes=[
            pltpu.VMEM((groups, DK, wide), HALF),
            pltpu.VMEM((groups, DK, local_heads * DV), HALF),
            pltpu.VMEM((groups, DK, local_heads * DV), HALF),
            pltpu.VMEM((tok_rows, head_count * DV), HALF),
            pltpu.VMEM(out_weight.shape, HALF),
            pltpu.SemaphoreType.DMA,
            pltpu.SemaphoreType.DMA,
        ]
        + [pltpu.SemaphoreType.DMA((groups,))] * 4,
        compiler_params=pltpu.CompilerParams(
            collective_id=0, has_side_effects=True, vmem_limit_bytes=60 * 1024 * 1024
        ),
        name="state",
    )(
        pairs, partial, reads, head_gain.reshape(1, DV), out_weight, residual[0],
        mix_gain.reshape(1, width), ffn_gain.reshape(1, width),
    )
    experts = lax.axis_size("sp") * lax.axis_size("dp")
    capacity = max(2, 2 * tok_rows * TOPK // experts)
    members = lax.axis_size("dp")
    if capacity % 16 == 0 and not (groups & (groups - 1)) and not (members & (members - 1)):
        hidden_units = w_gate.shape[2]
        block = pltpu.VMEM((experts, capacity, width), HALF)
        mixed = pl.pallas_call(
            functools.partial(expert_kernel, groups, members, capacity),
            out_shape=jax.ShapeDtypeStruct((tok_rows, width), HALF),
            in_specs=[VMEM] * 5 + [ANY] * 3,
            out_specs=VMEM,
            scratch_shapes=[
                block, block, block, block,
                pltpu.VMEM((width, hidden_units), HALF),
                pltpu.VMEM((width, hidden_units), HALF),
                pltpu.VMEM((hidden_units, width), HALF),
                pltpu.SemaphoreType.DMA((3,)),
                pltpu.SemaphoreType.DMA,
            ]
            + [pltpu.SemaphoreType.DMA((experts,))] * 4,
            compiler_params=pltpu.CompilerParams(
                collective_id=1, has_side_effects=True, vmem_limit_bytes=60 * 1024 * 1024
            ),
            name="experts",
        )(
            normed, hidden_state, route[0], route_weight[0], out_gain.reshape(1, width),
            w_gate[0], w_up[0], w_down[0],
        )
        return mixed[None]
    route_ids = route.reshape(tok_rows * TOPK)
    matches = (route_ids[:, None] == jnp.arange(experts, dtype=jnp.int32)).astype(jnp.int32)
    slot_index = jnp.sum((jnp.cumsum(matches, axis=0) - 1) * matches, axis=-1)
    target = route_ids * capacity + slot_index
    copies = jnp.repeat(normed, TOPK, axis=0)
    outgoing = jnp.zeros((experts * capacity, width), jnp.bfloat16).at[target].set(copies)
    arrived_block = lax.all_to_all(
        outgoing.reshape(experts, capacity, width),
        ("sp", "dp"),
        split_axis=0,
        concat_axis=0,
        tiled=True,
    )
    block_shape = arrived_block.shape
    flat_rows = arrived_block.reshape(-1, block_shape[-1])
    served = expert_ffn(flat_rows, w_gate[0], w_up[0], w_down[0]).reshape(block_shape)
    returned = lax.all_to_all(served, ("sp", "dp"), split_axis=0, concat_axis=0, tiled=True)
    gathered = returned.reshape(experts * capacity, width)[target].reshape(tok_rows, TOPK, width)
    combined = jnp.sum(
        route_weight.reshape(tok_rows, TOPK, 1) * gathered.astype(jnp.float32), axis=1
    )
    mixed = (hidden_state.astype(jnp.float32) + scale_rows(combined, out_gain)).astype(jnp.bfloat16)
    return mixed.reshape(1, tok_rows, width)


def solution(mesh):
    in_specs = (
        P("dp", "sp", None),
        P("dp", "sp", None),
        P("dp", "sp", None),
        P("dp", "sp", None),
        P("dp", "sp", None),
        P(),
        P(),
        P(),
        P("dp", "sp", None),
        P(),
        P(),
        P("dp", "sp", None),
        P("dp", "sp", None),
        P(("sp", "dp"), None, None),
        P(("sp", "dp"), None, None),
        P(("sp", "dp"), None, None),
        P(),
    )
    out_specs = P("dp", "sp", None)
    return jax.shard_map(local, mesh=mesh, in_specs=in_specs, out_specs=out_specs, check_vma=False)
```

```python
import functools

import jax
import jax.numpy as jnp
from jax import lax
from jax.experimental import pallas as pl
from jax.experimental.pallas import tpu as pltpu
from jax.sharding import PartitionSpec as P

DK = 64
DV = 128
TOPK = 2
BLOCK = 128
EPSILON = 1e-06
PRECISE = lax.Precision.HIGHEST
MESH = pl.DeviceIdType.MESH
VMEM = pl.BlockSpec(memory_space=pltpu.VMEM)
ANY = pl.BlockSpec(memory_space=pl.ANY)
HALF = jnp.bfloat16
NN = (((1,), (0,)), ((), ()))
NT = (((1,), (1,)), ((), ()))
TN = (((0,), (0,)), ((), ()))


def dot(a, b, dims=NN, precision=None):
    return lax.dot_general(a, b, dims, precision=precision, preferred_element_type=jnp.float32)


def unit_rows(x):
    return x * lax.rsqrt(jnp.sum(x * x, axis=-1, keepdims=True) + EPSILON)


def scale_rows(x, gain):
    return x * lax.rsqrt(jnp.mean(x * x, axis=-1, keepdims=True) + EPSILON) * gain


def pair_width(local_heads):
    return max(DV, local_heads * DK)


def block_kernel(groups, local_heads, q_ref, k_ref, v_ref, decay_ref, mix_ref, rates_ref, ab_ref, o_ref, qe_ref):
    length = q_ref.shape[0]
    heads = groups * local_heads
    rows = lax.broadcasted_iota(jnp.int32, (length, length), 0)
    cols = lax.broadcasted_iota(jnp.int32, (length, length), 1)
    lower = rows >= cols
    strict = rows > cols
    decay = decay_ref[...].astype(jnp.float32)
    softplus = jnp.maximum(decay, 0.0) + jnp.log1p(jnp.exp(-jnp.abs(decay)))
    beta = 1.0 / (1.0 + jnp.exp(-mix_ref[...].astype(jnp.float32)))
    beta = dot((rows == cols).astype(jnp.float32), beta, NT, PRECISE)
    running = dot(lower.astype(jnp.float32), softplus, NT, PRECISE) * -rates_ref[...]
    spot_r = lax.broadcasted_iota(jnp.int32, (heads, heads), 0)
    spot_c = lax.broadcasted_iota(jnp.int32, (heads, heads), 1)
    running_t = dot((spot_r == spot_c).astype(jnp.float32), running, NT, PRECISE)
    grow = jnp.exp(running)
    total = running[length - 1 : length, :]
    shrink = jnp.exp(total - running)
    whole = jnp.exp(total)
    eye = (
        lax.broadcasted_iota(jnp.int32, (DK, DK), 0) == lax.broadcasted_iota(jnp.int32, (DK, DK), 1)
    ).astype(jnp.float32)
    scale = DK ** (-0.5)
    batch = 8 if heads % 8 == 0 else 1
    base = pair_width(local_heads)
    for first in range(0, heads, batch):
        own = range(first, first + batch)
        work = []
        for h in own:
            qn = unit_rows(q_ref[:, h * DK : (h + 1) * DK].astype(jnp.float32)).astype(HALF)
            kn = unit_rows(k_ref[:, h * DK : (h + 1) * DK].astype(jnp.float32)).astype(HALF)
            spread = running[:, h : h + 1] - running_t[h : h + 1, :]
            tile = jnp.where(lower, jnp.exp(jnp.where(lower, spread, 0.0)), 0.0)
            bet = beta[:, h : h + 1]
            strict_part = jnp.where(strict, dot(kn, kn, NT) * bet * tile, 0.0)
            scores = (dot(qn, kn, NT) * scale * tile).astype(HALF)
            work.append((qn, kn, strict_part, scores))
        size = 1
        inverses = [None] * batch
        while size < length:
            joins = (rows // (2 * size) == cols // (2 * size)) & ((rows // size) % 2 == 1) & ((cols // size) % 2 == 0)
            for i in range(batch):
                part = jnp.where(joins, work[i][2], 0.0)
                if size == 1:
                    inverses[i] = (rows == cols).astype(jnp.float32) - part
                else:
                    half = inverses[i].astype(HALF)
                    step = dot(part.astype(HALF), half)
                    inverses[i] = inverses[i] - dot(half, step.astype(HALF))
            size *= 2
        for i, h in enumerate(own):
            qn, kn, strict_part, scores = work[i]
            bet = beta[:, h : h + 1]
            key = kn.astype(jnp.float32)
            values = v_ref[:, h * DV : (h + 1) * DV].astype(jnp.float32) * bet
            inputs = jnp.concatenate([values, key * (bet * grow[:, h : h + 1])], axis=1)
            solved = dot(inverses[i].astype(HALF), inputs.astype(HALF))
            solved = solved.astype(HALF)
            seen = dot(scores, solved)
            kept = dot((key * shrink[:, h : h + 1]).astype(HALF), solved, TN)
            o_ref[:, h * DV : (h + 1) * DV] = seen[:, :DV]
            query = qn.astype(jnp.float32) * (scale * grow[:, h : h + 1])
            qe_ref[h] = (query - seen[:, DV:]).astype(HALF)
            owner, place = h // local_heads, h % local_heads
            ab_ref[owner, :, base + place * DV : base + (place + 1) * DV] = kept[:, :DV].astype(HALF)
            ab_ref[owner, :, place * DK : (place + 1) * DK] = (
                eye * whole[:, h : h + 1] - kept[:, DV:]
            ).astype(HALF)
            if local_heads * DK < base and place == local_heads - 1:
                ab_ref[owner, :, local_heads * DK : base] = jnp.zeros((DK, base - local_heads * DK), HALF)


def state_kernel(
    groups, local_heads, fused,
    ab_ref, o_ref, qe_ref, hg_ref, w_hbm, res_ref, mg_ref, fg_ref,
    hidden_ref, normed_ref,
    ab_in, s_out, s_in, att, w_ref,
    w_sem, own_sem, send1, recv1, send2, recv2,
):
    me = lax.axis_index("sp")
    fetch = pltpu.make_async_copy(w_hbm, w_ref, w_sem)
    if not fused:
        fetch.start()
        barrier = pltpu.get_barrier_semaphore()
        for step in range(1, groups):
            pl.semaphore_signal(barrier, inc=1, device_id={"sp": lax.rem(me + step, groups)}, device_id_type=MESH)
        pl.semaphore_wait(barrier, groups - 1)

    def first_copy(step):
        peer = lax.rem(me + step, groups)
        return pltpu.make_async_remote_copy(
            src_ref=ab_ref.at[peer], dst_ref=ab_in.at[me],
            send_sem=send1.at[step], recv_sem=recv1.at[step],
            device_id={"sp": peer}, device_id_type=MESH,
        )

    def second_copy(step):
        peer = lax.rem(me + step, groups)
        return pltpu.make_async_remote_copy(
            src_ref=s_out.at[peer], dst_ref=s_in.at[me],
            send_sem=send2.at[step], recv_sem=recv2.at[step],
            device_id={"sp": peer}, device_id_type=MESH,
        )

    for step in range(1, groups):
        first_copy(step).start()
    own = pltpu.make_async_copy(ab_ref.at[me], ab_in.at[me], own_sem)
    own.start()
    own.wait()
    for step in range(1, groups):
        first_copy(step).wait()
    base = pair_width(local_heads)
    states = [jnp.zeros((DK, DV), jnp.float32)] * local_heads
    for block in range(groups):
        for place in range(local_heads):
            half = states[place].astype(HALF)
            s_out[block, :, place * DV : (place + 1) * DV] = half
            if block < groups - 1:
                states[place] = (
                    dot(ab_in[block, :, place * DK : (place + 1) * DK], half)
                    + ab_in[block, :, base + place * DV : base + (place + 1) * DV].astype(jnp.float32)
                )
    for step in range(1, groups):
        second_copy(step).start()
    own = pltpu.make_async_copy(s_out.at[me], s_in.at[me], own_sem)
    own.start()
    own.wait()
    for step in range(1, groups):
        second_copy(step).wait()
    for h in range(groups * local_heads):
        owner, place = h // local_heads, h % local_heads
        state = s_in[owner, :, place * DV : (place + 1) * DV]
        out = o_ref[:, h * DV : (h + 1) * DV] + dot(qe_ref[h], state)
        att[:, h * DV : (h + 1) * DV] = scale_rows(out, hg_ref[...]).astype(HALF)
    fetch.wait()
    projected = dot(att[...], w_ref[...])
    hidden = (res_ref[...].astype(jnp.float32) + scale_rows(projected, mg_ref[...])).astype(HALF)
    hidden_ref[...] = hidden
    normed_ref[...] = scale_rows(hidden.astype(jnp.float32), fg_ref[...]).astype(HALF)


def flip(index, mask, bits):
    result = 0
    for bit in range(bits):
        own = (index // (1 << bit)) % 2
        other = (mask // (1 << bit)) % 2
        result = result + (own + other - 2 * own * other) * (1 << bit)
    return result


def expert_kernel(
    groups, members, capacity,
    normed_ref, hidden_ref, route_ref, share_ref, gain_ref, gate_hbm, up_hbm, down_hbm,
    mixed_ref,
    outgoing, arrived, served, returned, gate_ref, up_ref, down_ref,
    w_sems, own_sem, send1, recv1, send2, recv2,
):
    sp, dp = lax.axis_index("sp"), lax.axis_index("dp")
    count = groups * members
    sp_bits, dp_bits = groups.bit_length() - 1, members.bit_length() - 1
    def masks(k):
        mask = count - 1 - k
        return mask // members, mask % members

    def partner(k):
        sp_mask, dp_mask = masks(k)
        return {"sp": flip(sp, sp_mask, sp_bits), "dp": flip(dp, dp_mask, dp_bits)}

    tokens = normed_ref.shape[0]
    slots = count * capacity
    names = lax.broadcasted_iota(jnp.int32, (count, tokens), 0)
    first, second = route_ref[0:1, :] == names, route_ref[1:2, :] == names
    both = first.astype(jnp.float32) + second.astype(jnp.float32)
    rows = lax.broadcasted_iota(jnp.int32, (tokens, tokens), 0)
    cols = lax.broadcasted_iota(jnp.int32, (tokens, tokens), 1)
    before = dot(both.astype(HALF), (rows > cols).astype(HALF), NT)
    places_t = (both * (before + 1.0)).astype(HALF)
    share_t = first.astype(jnp.float32) * share_ref[0:1, :] + second.astype(jnp.float32) * share_ref[1:2, :]
    high_t = share_t.astype(HALF)
    low_t = (share_t - high_t.astype(jnp.float32)).astype(HALF)
    turned = (rows == cols).astype(HALF)
    places, share_high, share_low = (dot(turned, x, NT).astype(HALF) for x in (places_t, high_t, low_t))

    def owner_of(slot):
        sp_mask, dp_mask = masks(slot // capacity)
        return flip(sp, sp_mask, sp_bits) * members + flip(dp, dp_mask, dp_bits)

    down_slot = lax.broadcasted_iota(jnp.int32, (slots, count), 0)
    spread_rows = (owner_of(down_slot) == lax.broadcasted_iota(jnp.int32, (slots, count), 1)).astype(HALF)
    turn = (lax.broadcasted_iota(jnp.int32, (slots, tokens), 0) % capacity + 1).astype(jnp.float32)
    pick = (dot(spread_rows, places_t) == turn).astype(HALF)
    normed = normed_ref[...]
    width = normed.shape[1]
    chunk = slots // 4 if slots % (4 * capacity) == 0 else slots
    per = chunk // capacity
    def go(k):
        return pltpu.make_async_remote_copy(
            src_ref=outgoing.at[k], dst_ref=arrived.at[k],
            send_sem=send1.at[k], recv_sem=recv1.at[k],
            device_id=partner(k), device_id_type=MESH,
        )

    def back(k):
        return pltpu.make_async_remote_copy(
            src_ref=served.at[k], dst_ref=returned.at[k],
            send_sem=send2.at[k], recv_sem=recv2.at[k],
            device_id=partner(k), device_id_type=MESH,
        )

    for at in range(0, slots, chunk):
        block = dot(pick[at : at + chunk], normed).astype(HALF)
        outgoing[at // capacity : at // capacity + per] = block.reshape(per, capacity, width)
        for k in range(at // capacity, min(at // capacity + per, count - 1)):
            go(k).start()
    own = pltpu.make_async_copy(outgoing.at[count - 1], arrived.at[count - 1], own_sem)
    own.start()
    own.wait()
    match = dot(places, spread_rows, NT) == (
        lax.broadcasted_iota(jnp.int32, (tokens, slots), 1) % capacity + 1
    ).astype(jnp.float32)
    high = jnp.where(match, dot(share_high, spread_rows, NT), 0.0).astype(HALF)
    low = jnp.where(match, dot(share_low, spread_rows, NT), 0.0).astype(HALF)
    for i, (source, target) in enumerate(((gate_hbm, gate_ref), (up_hbm, up_ref), (down_hbm, down_ref))):
        pltpu.make_async_copy(source, target, w_sems.at[i]).wait()
    for at in range(0, count, per):
        for k in range(at, min(at + per, count - 1)):
            go(k).wait()
        rows_in = arrived[at : at + per].reshape(chunk, width)
        gate = dot(rows_in, gate_ref[...])
        inner = (gate / (1.0 + jnp.exp(-gate)) * dot(rows_in, up_ref[...])).astype(HALF)
        served[at : at + per] = dot(inner, down_ref[...]).astype(HALF).reshape(per, capacity, width)
        for k in range(at, min(at + per, count - 1)):
            back(k).start()
    own = pltpu.make_async_copy(served.at[count - 1], returned.at[count - 1], own_sem)
    own.start()
    own.wait()
    total = jnp.zeros((tokens, width), jnp.float32)
    for at in range(0, count, per):
        for k in range(at, min(at + per, count - 1)):
            back(k).wait()
        block = returned[at : at + per].reshape(chunk, width)
        low_slot, high_slot = at * capacity, at * capacity + chunk
        total = total + dot(high[:, low_slot:high_slot], block) + dot(low[:, low_slot:high_slot], block)
    mixed_ref[...] = (hidden_ref[...].astype(jnp.float32) + scale_rows(total, gain_ref[...])).astype(HALF)


def layer_kernel(
    groups, members, local_heads, capacity,
    q_ref, k_ref, v_ref, decay_ref, mix_ref, rates_ref,
    hg_ref, w_hbm, res_ref, mg_ref, fg_ref,
    route_ref, share_ref, gain_ref, gate_hbm, up_hbm, down_hbm,
    mixed_ref,
    ab_ref, o_ref, qe_ref, hidden_ref, normed_ref,
    ab_in, s_out, s_in, att, w_ref, w_sem, own_sem, send1, recv1, send2, recv2,
    outgoing, arrived, served, returned, gate_ref, up_ref, down_ref,
    w_sems, own_sem2, send3, recv3, send4, recv4,
):
    sp, dp = lax.axis_index("sp"), lax.axis_index("dp")
    barrier = pltpu.get_barrier_semaphore()
    for step in range(1, groups * members):
        there = {"sp": lax.rem(sp + step // members, groups), "dp": lax.rem(dp + step % members, members)}
        pl.semaphore_signal(barrier, inc=1, device_id=there, device_id_type=MESH)
    pltpu.make_async_copy(w_hbm, w_ref, w_sem).start()
    for i, (source, target) in enumerate(((gate_hbm, gate_ref), (up_hbm, up_ref), (down_hbm, down_ref))):
        pltpu.make_async_copy(source, target, w_sems.at[i]).start()
    block_kernel(
        groups, local_heads, q_ref, k_ref, v_ref, decay_ref, mix_ref, rates_ref, ab_ref, o_ref, qe_ref
    )
    pl.semaphore_wait(barrier, groups * members - 1)
    state_kernel(
        groups, local_heads, True,
        ab_ref, o_ref, qe_ref, hg_ref, w_hbm, res_ref, mg_ref, fg_ref,
        hidden_ref, normed_ref,
        ab_in, s_out, s_in, att, w_ref,
        w_sem, own_sem, send1, recv1, send2, recv2,
    )
    expert_kernel(
        groups, members, capacity,
        normed_ref, hidden_ref, route_ref, share_ref, gain_ref, gate_hbm, up_hbm, down_hbm,
        mixed_ref,
        outgoing, arrived, served, returned, gate_ref, up_ref, down_ref,
        w_sems, own_sem2, send3, recv3, send4, recv4,
    )


def expert_ffn(rows_in, gate_weight, up_weight, down_weight):
    gate = jnp.dot(rows_in, gate_weight, preferred_element_type=jnp.float32)
    upward = jnp.dot(rows_in, up_weight, preferred_element_type=jnp.float32)
    inner = (jax.nn.silu(gate) * upward).astype(jnp.bfloat16)
    return jnp.dot(inner, down_weight, preferred_element_type=jnp.float32).astype(jnp.bfloat16)


def local(
    queries,
    keys,
    values,
    decay_in,
    mix_in,
    rates,
    head_gain,
    out_weight,
    residual,
    mix_gain,
    ffn_gain,
    route,
    route_weight,
    w_gate,
    w_up,
    w_down,
    out_gain,
):
    groups = lax.axis_size("sp")
    tok_rows = queries.shape[1]
    head_count = rates.shape[0]
    local_heads = head_count // groups
    width = out_weight.shape[1]
    wide = pair_width(local_heads) + local_heads * DV
    members = lax.axis_size("dp")
    experts = groups * members
    capacity = max(2, 2 * tok_rows * TOPK // experts)
    if capacity % 16 == 0 and not (groups & (groups - 1)) and not (members & (members - 1)):
        hidden_units = w_gate.shape[2]
        block = pltpu.VMEM((experts, capacity, width), HALF)
        states = pltpu.VMEM((groups, DK, local_heads * DV), HALF)
        mixed = pl.pallas_call(
            functools.partial(layer_kernel, groups, members, local_heads, capacity),
            out_shape=jax.ShapeDtypeStruct((tok_rows, width), HALF),
            in_specs=[VMEM] * 7 + [ANY] + [VMEM] * 6 + [ANY] * 3,
            out_specs=VMEM,
            scratch_shapes=[
                pltpu.VMEM((groups, DK, wide), HALF),
                pltpu.VMEM((tok_rows, head_count * DV), jnp.float32),
                pltpu.VMEM((head_count, tok_rows, DK), HALF),
                pltpu.VMEM((tok_rows, width), HALF),
                pltpu.VMEM((tok_rows, width), HALF),
                pltpu.VMEM((groups, DK, wide), HALF),
                states, states,
                pltpu.VMEM((tok_rows, head_count * DV), HALF),
                pltpu.VMEM(out_weight.shape, HALF),
                pltpu.SemaphoreType.DMA,
                pltpu.SemaphoreType.DMA,
            ]
            + [pltpu.SemaphoreType.DMA((groups,))] * 4
            + [
                block, block, block, block,
                pltpu.VMEM((width, hidden_units), HALF),
                pltpu.VMEM((width, hidden_units), HALF),
                pltpu.VMEM((hidden_units, width), HALF),
                pltpu.SemaphoreType.DMA((3,)),
                pltpu.SemaphoreType.DMA,
            ]
            + [pltpu.SemaphoreType.DMA((experts,))] * 4,
            compiler_params=pltpu.CompilerParams(
                collective_id=0, has_side_effects=True, vmem_limit_bytes=60 * 1024 * 1024
            ),
            name="layer",
        )(
            queries[0], keys[0], values[0], decay_in[0].T, mix_in[0].T, rates.reshape(1, head_count),
            head_gain.reshape(1, DV), out_weight, residual[0],
            mix_gain.reshape(1, width), ffn_gain.reshape(1, width),
            route[0].T, route_weight[0].T, out_gain.reshape(1, width),
            w_gate[0], w_up[0], w_down[0],
        )
        return mixed[None]
    pairs, partial, reads = pl.pallas_call(
        functools.partial(block_kernel, groups, local_heads),
        out_shape=(
            jax.ShapeDtypeStruct((groups, DK, wide), HALF),
            jax.ShapeDtypeStruct((tok_rows, head_count * DV), jnp.float32),
            jax.ShapeDtypeStruct((head_count, tok_rows, DK), HALF),
        ),
        in_specs=[VMEM] * 6,
        out_specs=(VMEM,) * 3,
        compiler_params=pltpu.CompilerParams(vmem_limit_bytes=60 * 1024 * 1024),
        name="block",
    )(queries[0], keys[0], values[0], decay_in[0].T, mix_in[0].T, rates.reshape(1, head_count))
    hidden_state, normed = pl.pallas_call(
        functools.partial(state_kernel, groups, local_heads, False),
        out_shape=(jax.ShapeDtypeStruct((tok_rows, width), HALF),) * 2,
        in_specs=[VMEM] * 4 + [ANY] + [VMEM] * 3,
        out_specs=(VMEM,) * 2,
        scratch_shapes=[
            pltpu.VMEM((groups, DK, wide), HALF),
            pltpu.VMEM((groups, DK, local_heads * DV), HALF),
            pltpu.VMEM((groups, DK, local_heads * DV), HALF),
            pltpu.VMEM((tok_rows, head_count * DV), HALF),
            pltpu.VMEM(out_weight.shape, HALF),
            pltpu.SemaphoreType.DMA,
            pltpu.SemaphoreType.DMA,
        ]
        + [pltpu.SemaphoreType.DMA((groups,))] * 4,
        compiler_params=pltpu.CompilerParams(
            collective_id=0, has_side_effects=True, vmem_limit_bytes=60 * 1024 * 1024
        ),
        name="state",
    )(
        pairs, partial, reads, head_gain.reshape(1, DV), out_weight, residual[0],
        mix_gain.reshape(1, width), ffn_gain.reshape(1, width),
    )
    route_ids = route.reshape(tok_rows * TOPK)
    matches = (route_ids[:, None] == jnp.arange(experts, dtype=jnp.int32)).astype(jnp.int32)
    slot_index = jnp.sum((jnp.cumsum(matches, axis=0) - 1) * matches, axis=-1)
    target = route_ids * capacity + slot_index
    copies = jnp.repeat(normed, TOPK, axis=0)
    outgoing = jnp.zeros((experts * capacity, width), jnp.bfloat16).at[target].set(copies)
    arrived_block = lax.all_to_all(
        outgoing.reshape(experts, capacity, width),
        ("sp", "dp"),
        split_axis=0,
        concat_axis=0,
        tiled=True,
    )
    block_shape = arrived_block.shape
    flat_rows = arrived_block.reshape(-1, block_shape[-1])
    served = expert_ffn(flat_rows, w_gate[0], w_up[0], w_down[0]).reshape(block_shape)
    returned = lax.all_to_all(served, ("sp", "dp"), split_axis=0, concat_axis=0, tiled=True)
    gathered = returned.reshape(experts * capacity, width)[target].reshape(tok_rows, TOPK, width)
    combined = jnp.sum(
        route_weight.reshape(tok_rows, TOPK, 1) * gathered.astype(jnp.float32), axis=1
    )
    mixed = (hidden_state.astype(jnp.float32) + scale_rows(combined, out_gain)).astype(jnp.bfloat16)
    return mixed.reshape(1, tok_rows, width)


def solution(mesh):
    in_specs = (
        P("dp", "sp", None),
        P("dp", "sp", None),
        P("dp", "sp", None),
        P("dp", "sp", None),
        P("dp", "sp", None),
        P(),
        P(),
        P(),
        P("dp", "sp", None),
        P(),
        P(),
        P("dp", "sp", None),
        P("dp", "sp", None),
        P(("sp", "dp"), None, None),
        P(("sp", "dp"), None, None),
        P(("sp", "dp"), None, None),
        P(),
    )
    out_specs = P("dp", "sp", None)
    return jax.shard_map(local, mesh=mesh, in_specs=in_specs, out_specs=out_specs, check_vma=False)
```
